32 devices in a mesh: ep: 8 (over z, x), tp: 4 (over y, core).
Axes of the slice: x: 2, y: 2, z: 4, core: 2. Of those that a mesh axis runs over, the one named last changes fastest.
Arguments:
- out_gate: bfloat16 [4096, 2048], P(('ep', 'tp')), may hold values from -6 to 6
- in_gate: bfloat16 [4096, 2048], P(('ep', 'tp')), may hold values from -6 to 6
- values: bfloat16 [4096, 2048], P(('ep', 'tp')), may hold values from -6 to 6
- conv_taps: float32 [3, 2048], replicated, may hold values from -4 to 4
- out_weight: bfloat16 [2048, 2048], P(None, 'tp'), may hold values from -0.125 to 0.125
- expert_input: bfloat16 [8192, 2048], P(('ep', 'tp')), may hold values from -6 to 6
- norm_gain: float32 [2048], replicated, may hold values from 0.1 to 1.9
- expert_ids: int32 [8192, 2], P(('ep', 'tp')), may hold values from 0 to 7, all different within a row; in each aligned block of 256 rows (0 to 255, 256 to 511, ...) at most 128 rows name the same one
- route_logits: float32 [8192, 2], P(('ep', 'tp')), may hold values from -8 to 8
- group_share: float32 [8192], P(('ep', 'tp')), may hold values from 0.3 to 1
- gate_weight: bfloat16 [8, 2048, 512], P('ep'), may hold values from -0.125 to 0.125
- up_weight: bfloat16 [8, 2048, 512], P('ep'), may hold values from -0.125 to 0.125
- down_weight: bfloat16 [8, 512, 2048], P('ep'), may hold values from -0.25 to 0.25
Outputs:
- mixer_out: bfloat16 [4096, 2048], P(('ep', 'tp'))
- expert_mix: bfloat16 [8192, 2048], P(('ep', 'tp'))
The draws below stay inside these ranges and needn't reach their ends.
Inputs may be any that keep to these rules, and one draw needn't show every extreme that they name: `expert_ids`: each row names 2 different experts. Within the rows of one device (aligned blocks of 256 rows) no expert is named by more than 128 rows, a bound that some block reaches.
All inputs are finite; a program needn't handle non-finite values.
Results may differ from the reference program's by a relative error of at most 0.0071.
Values may be sent and summed in bfloat16 or wider, within the bound.
No kernel may reach another device: no remote copies, remote signals or barrier semaphores. Data moves between devices by JAX's collectives and lax.ppermute only.
A program may use at most 128 MiB of HBM per device.

```python
import math
import jax
import jax.numpy as jnp
import numpy as np
from jax import lax

D = 2048
F = 512
EXPERTS = 8
TOP = 2
CONV = 3
SEQS = 1
TOK_B = 256
TOKENS_A = 4096
TOKENS_B = 8192
CAP = 128
N_EP = 8
N_TP = 4


def levels(stream_key, dims, pieces, least, high):
    def one(axis_at, blocks):
        heights = jax.random.uniform(jax.random.fold_in(jax.random.fold_in(stream_key, 6), axis_at), (blocks,), jnp.float32, least / len(pieces), high / len(pieces))
        return jnp.repeat(jnp.exp(heights), dims[axis_at] // blocks).reshape((-1,) + (1,) * (len(dims) - axis_at - 1))

    loudness = one(*pieces[0])
    for cut in pieces[1:]:
        loudness = loudness * one(*cut)
    return loudness


def shared_out(stream_key, own, number, rows, amount, top, reach, slope):
    ranking = jax.random.permutation(stream_key, amount)
    heavy_load, common = shares(amount, rows * top, reach, slope, True), shares(amount, rows * top, reach, slope, False)
    places = jnp.arange(amount)

    def named(lengths, rotation):
        used = int((lengths > 0).sum())
        fixed = max(1, used // 4)
        shifted = fixed + (places - fixed + rotation * (used - fixed)) % max(1, amount - fixed)
        return jnp.zeros((amount,), jnp.int32).at[ranking[jnp.where(places < fixed, places, shifted)]].set(jnp.asarray(lengths, jnp.int32))

    lengths = jnp.where(number % 4 == 0, named(heavy_load, number // 4), named(common, number - number // 4 - 1))
    mixed = jax.random.permutation(jax.random.fold_in(own, 3), amount)
    giver, receiver = mixed[0:amount // 2 * 2:2], mixed[1:amount // 2 * 2:2]
    room = jnp.minimum(lengths[giver] - 1, reach - lengths[receiver]) // 2
    room = jnp.where((giver == ranking[0]) | (receiver == ranking[0]) | (lengths[receiver] == 0), 0, jnp.maximum(room, 0))
    shifted = jax.random.randint(jax.random.fold_in(own, 4), (amount // 2,), 0, 1 << 20) % (room + 1)
    lengths = lengths.at[giver].add(-shifted).at[receiver].add(shifted)
    items = jnp.searchsorted(jnp.cumsum(lengths), jnp.arange(rows * top), side="right").astype(jnp.int32)
    listing = items.reshape(top, rows).T
    listing = listing[jax.random.permutation(jax.random.fold_in(own, 1), rows)]
    rotation = jax.random.randint(jax.random.fold_in(own, 2), (rows, 1), 0, top)
    return jnp.take_along_axis(listing, (jnp.arange(top)[None, :] + rotation) % top, axis=1)


def shares(number_of, total, most, skew, full):
    loads = [(1 << 20) // math.isqrt(grade ** skew) + 1 for grade in range(1, number_of + 1)]
    largest = most if full else min(most, max(-(-total // number_of), total * loads[0] // sum(loads)))
    least = 1 if total - largest >= number_of - 1 else 0
    given, spare = [largest] + [least] * (number_of - 1), total - largest - least * (number_of - 1)
    while spare > 0:
        candidates = [i for i in range(1, number_of) if given[i] < largest] or [i for i in range(1, number_of) if given[i] < most]
        mass, left = sum([loads[i] for i in candidates]), spare
        for i in candidates:
            more = min(most - given[i], max(1, left * loads[i] // mass), spare)
            given[i] = given[i] + more
            spare = spare - more
    return np.array(given)


def scatter_about(key, dims, scale, limit, pieces=(), kind=jnp.bfloat16):
    factor_of = levels(key, dims, pieces, -0.22, 0.18) if pieces else 1.0
    values = jax.random.normal(key, dims, jnp.float32) * scale * factor_of
    return jnp.minimum(jnp.maximum(values, -limit), limit).astype(kind)


def setup_inputs(seed: int = 0) -> dict:
    streams_of = jax.random.split(jax.random.key(seed), 14)
    out_gate = scatter_about(streams_of[0], (TOKENS_A, D), 1.0, 6.0, ((0, 32),))
    in_gate = scatter_about(streams_of[1], (TOKENS_A, D), 1.0, 6.0, ((0, 32),))
    values = scatter_about(streams_of[2], (TOKENS_A, D), 1.0, 6.0, ((0, 32),))
    conv_taps = scatter_about(streams_of[3], (CONV, D), 0.6, 4.0, (), jnp.float32)
    out_weight = scatter_about(streams_of[4], (D, D), D ** -0.5, 0.125, ((1, 4),))
    expert_input = scatter_about(streams_of[5], (TOKENS_B, D), 1.0, 6.0, ((0, 32),))
    norm_gain = jnp.clip(1.0 + 0.18 * jax.random.normal(streams_of[6], (D,), jnp.float32), 0.1, 1.9)
    expert_ids_keys = jax.random.split(jax.random.fold_in(streams_of[7], 1), TOKENS_B // TOK_B)
    expert_ids_turns = jax.random.permutation(jax.random.fold_in(streams_of[7], 3), TOKENS_B // TOK_B)
    expert_ids = jax.vmap(lambda own, number: shared_out(jax.random.fold_in(streams_of[7], 2), own, number, TOK_B, EXPERTS, TOP, CAP, 2))(expert_ids_keys, expert_ids_turns).reshape((TOKENS_B, TOP))
    route_logits = scatter_about(streams_of[8], (TOKENS_B, TOP), 1.5, 8.0, ((0, 32),), jnp.float32)
    group_share = jnp.clip(0.3 + 0.7 * jax.random.uniform(streams_of[9], (TOKENS_B,), jnp.float32) ** levels(streams_of[9], (TOKENS_B,), ((0, 32),), -0.2, 0.2), 0.3, 1.0)
    gate_weight = scatter_about(streams_of[10], (EXPERTS, D, F), D ** -0.5, 0.125, ((0, 8),))
    up_weight = scatter_about(streams_of[11], (EXPERTS, D, F), D ** -0.5, 0.125, ((0, 8),))
    down_weight = scatter_about(streams_of[12], (EXPERTS, F, D), F ** -0.5, 0.25, ((0, 8),))
    return {"out_gate": out_gate, "in_gate": in_gate, "values": values, "conv_taps": conv_taps, "out_weight": out_weight, "expert_input": expert_input, "norm_gain": norm_gain, "expert_ids": expert_ids, "route_logits": route_logits, "group_share": group_share, "gate_weight": gate_weight, "up_weight": up_weight, "down_weight": down_weight}


norm_eps = 1e-05

def reference(out_gate, in_gate, values, conv_taps, out_weight, expert_input, norm_gain, expert_ids, route_logits, group_share, gate_weight, up_weight, down_weight):
    gated = (in_gate.astype(jnp.float32) * values.astype(jnp.float32)).astype(jnp.bfloat16)
    per_seq = gated.reshape(SEQS, -1, D).astype(jnp.float32)
    length = per_seq.shape[1]
    padded = jnp.pad(per_seq, ((0, 0), (CONV - 1, 0), (0, 0)))
    filtered = jnp.zeros_like(per_seq)
    for index in range(CONV):
        filtered = filtered + padded[:, index:index + length] * conv_taps[index]
    mixed_rows = (out_gate.astype(jnp.float32) * filtered.reshape(-1, D)).astype(jnp.bfloat16)
    mixer_out = jnp.dot(mixed_rows, out_weight, preferred_element_type=jnp.float32).astype(jnp.bfloat16)
    inputs = expert_input.astype(jnp.float32)
    scale = lax.rsqrt(lax.optimization_barrier(jnp.mean(inputs * inputs, axis=-1, keepdims=True)) + norm_eps)
    normed = (inputs * scale * norm_gain).astype(jnp.bfloat16)
    total = TOKENS_B * TOP
    flat_ids = expert_ids.reshape(-1).astype(jnp.int32)
    order = jnp.argsort(flat_ids, stable=True).astype(jnp.int32)
    counts = jax.ops.segment_sum(jnp.ones((total,), jnp.int32), flat_ids, EXPERTS).astype(jnp.int32)
    starts = (jnp.cumsum(counts) - counts).astype(jnp.int32)
    bound = N_EP * N_TP * CAP
    steps_in = jnp.arange(bound, dtype=jnp.int32)

    def per_expert(stored, expert):
        places = starts[expert] + steps_in
        valid = steps_in < counts[expert]
        entry = order[jnp.minimum(places, total - 1)]
        rows = normed[entry // TOP]
        gate = jnp.dot(rows, gate_weight[expert], preferred_element_type=jnp.float32)
        upper = jnp.dot(rows, up_weight[expert], preferred_element_type=jnp.float32)
        hidden = (jax.nn.silu(gate) * upper).astype(jnp.bfloat16)
        result = jnp.dot(hidden, down_weight[expert], preferred_element_type=jnp.float32).astype(jnp.bfloat16)
        target = jnp.where(valid, entry, total).astype(jnp.int32)
        return (stored.at[target].set(result, mode='drop'), None)
    stored = jnp.zeros((total, D), jnp.bfloat16)
    stored, _ = lax.scan(per_expert, stored, jnp.arange(EXPERTS, dtype=jnp.int32))
    expert_out = stored.reshape(TOKENS_B, TOP, D).astype(jnp.float32)
    margin = route_logits[:, 0] - route_logits[:, 1]
    route_weight = group_share[:, None] * jnp.stack([jax.nn.sigmoid(margin), jax.nn.sigmoid(-margin)], axis=1)
    expert_mix = lax.optimization_barrier(jnp.sum(expert_out * route_weight[:, :, None], axis=1)).astype(jnp.bfloat16)
    return (mixer_out, expert_mix)
```

```python
import functools
import math

import jax
import jax.numpy as jnp
from jax import lax
from jax.experimental import pallas as pl
from jax.experimental.pallas import tpu as pltpu
from jax.sharding import PartitionSpec as P

SEQS = 1

norm_eps = 1e-05

F32 = jnp.float32
BF16 = jnp.bfloat16
LANES = 128
VMEM_BYTES = 40 * 1024 * 1024


def plane_shape(ep):
    across = math.isqrt(ep // 2)
    if across < 1 or 2 * across * across != ep:
        across = 1
    return ep // across, across


def pack_weights(gate, up, down, part, parts):
    width, units = gate.shape
    share = units // parts
    half = width // 2
    step = 2 * share

    def body(_, gate_ref, up_ref, down_ref, low_ref, high_ref, out_ref):
        low_ref[:, :share] = gate_ref[:half, :]
        low_ref[:, share:] = up_ref[:half, :]
        high_ref[:, :share] = gate_ref[half:, :]
        high_ref[:, share:] = up_ref[half:, :]
        for i in range(width // step):
            out_ref[i * share : (i + 1) * share, :] = down_ref[:, i * step : (i + 1) * step]

    piece = jax.ShapeDtypeStruct((half, step), BF16)
    return pl.pallas_call(
        body,
        grid_spec=pltpu.PrefetchScalarGridSpec(
            num_scalar_prefetch=1,
            grid=(1,),
            in_specs=[
                pl.BlockSpec((width, share), lambda i, p: (0, p[0])),
                pl.BlockSpec((width, share), lambda i, p: (0, p[0])),
                pl.BlockSpec((share, width), lambda i, p: (p[0], 0)),
            ],
            out_specs=[pl.BlockSpec((half, step), lambda i, p: (0, 0))] * 3,
        ),
        out_shape=[piece] * 3,
        compiler_params=pltpu.CompilerParams(vmem_limit_bytes=16 * 1024 * 1024),
        name="pack_weights",
    )(part, gate, up, down)


def ffn(slots, scalars, experts, meta, gain, own, pieces):
    arrays = [array for slot in slots for array in slot]
    tokens, width = arrays[0].shape
    gate, up, down = own
    units = gate.shape[1]
    others = len(pieces)
    flat = [part for shares in pieces for share in shares for part in share]
    column = 2 * LANES

    def body(scalar_ref, expert_ref, *refs):
        in_refs = refs[: len(arrays)]
        meta_ref, gain_ref, gate_ref, up_ref, down_ref = refs[len(arrays) : len(arrays) + 5]
        rest = refs[len(arrays) + 5 :]
        piece_refs = rest[: len(flat)]
        out_refs = rest[len(flat) : len(flat) + len(slots)]
        normed_ref, hidden_ref = rest[len(flat) + len(slots) :]

        def block(x_ref, origin, out_ref):
            x = x_ref[...].astype(F32)
            scale = lax.rsqrt(jnp.mean(x * x, axis=-1, keepdims=True) + norm_eps)
            normed_ref[...] = (x * scale * gain_ref[...]).astype(BF16)
            info = meta_ref[origin]
            rows = []
            for j in range(others + 1):
                expert = expert_ref[j].astype(F32)
                rows.append(
                    jnp.where(info[0:1] == expert, info[2:3], 0.0)
                    + jnp.where(info[1:2] == expert, info[3:4], 0.0)
                )
            rows.append(jnp.zeros((LANES - others - 1, tokens), F32))
            weights = jnp.concatenate(rows, axis=0).T
            normed = normed_ref[...]
            first = jnp.dot(normed, gate_ref[...], preferred_element_type=F32)
            second = jnp.dot(normed, up_ref[...], preferred_element_type=F32)
            hidden_ref[:, :units] = (jax.nn.silu(first) * second * weights[:, 0:1]).astype(BF16)
            at = units
            k = 0
            half = width // 2
            for j in range(others):
                for low, high, _ in pieces[j]:
                    share = low.shape[1] // 2
                    both = jnp.dot(
                        normed_ref[:, :half], piece_refs[k][...], preferred_element_type=F32
                    ) + jnp.dot(
                        normed_ref[:, half:], piece_refs[k + 1][...], preferred_element_type=F32
                    )
                    value = jax.nn.silu(both[:, :share]) * both[:, share:]
                    hidden_ref[:, at : at + share] = (value * weights[:, j + 1 : j + 2]).astype(BF16)
                    at += share
                    k += 3
            for i in range(width // column):
                total = jnp.dot(
                    hidden_ref[:, :units],
                    down_ref[:, i * column : (i + 1) * column],
                    preferred_element_type=F32,
                )
                k = 0
                at = units
                for j in range(others):
                    stack = []
                    for low, high, _ in pieces[j]:
                        share = low.shape[1] // 2
                        step = 2 * share
                        if step == column:
                            stack.append(piece_refs[k + 2][i * share : (i + 1) * share, :])
                        k += 3
                    total += jnp.dot(
                        hidden_ref[:, at : at + units],
                        jnp.concatenate(stack, axis=0),
                        preferred_element_type=F32,
                    )
                    at += units
                out_ref[:, i * column : (i + 1) * column] = total.astype(BF16)

        at = 0
        for out_ref, slot in zip(out_refs, slots):
            for _ in slot:

                @pl.when(scalar_ref[2 * at] == 1)
                def _(x_ref=in_refs[at], at=at, out_ref=out_ref):
                    block(x_ref, scalar_ref[2 * at + 1], out_ref)

                at += 1

    inputs = [scalars, experts, *arrays, meta, gain, gate, up, down, *flat]
    vmem = pl.BlockSpec(memory_space=pltpu.VMEM)
    smem = pl.BlockSpec(memory_space=pltpu.SMEM)
    weight_count = (others + 1) * 3 * width * units
    return pl.pallas_call(
        body,
        in_specs=[smem, smem] + [vmem] * (len(inputs) - 2),
        out_specs=[vmem] * len(slots),
        out_shape=[jax.ShapeDtypeStruct((tokens, width), BF16)] * len(slots),
        scratch_shapes=[
            pltpu.VMEM((tokens, width), BF16),
            pltpu.VMEM((tokens, (others + 1) * units), BF16),
        ],
        compiler_params=pltpu.CompilerParams(vmem_limit_bytes=VMEM_BYTES),
        cost_estimate=pl.CostEstimate(
            flops=2 * tokens * weight_count * len(slots),
            bytes_accessed=2 * weight_count + 4 * tokens * width * len(slots),
            transcendentals=tokens * units * (others + 1) * len(slots),
        ),
        name="ffn",
    )(*inputs)


def mixer(out_gate, in_gate, values, conv_taps, out_weight):
    rows_mix, width = out_gate.shape
    extent = conv_taps.shape[0] - 1
    tp = lax.axis_size("tp")
    devices = lax.axis_size("ep") * tp
    gated = (in_gate.astype(F32) * values.astype(F32)).astype(BF16)
    before = lax.ppermute(
        gated[rows_mix - extent :], ("ep", "tp"), [(i, i + 1) for i in range(devices - 1)]
    )
    extended = jnp.concatenate([before, gated], axis=0)
    seq_len = devices * rows_mix // SEQS
    position = lax.axis_index(("ep", "tp")) * rows_mix + jnp.arange(rows_mix, dtype=jnp.int32)
    offset = position % seq_len
    filtered = jnp.zeros((rows_mix, width), F32)
    for delays in range(extent + 1):
        lagged = extended[extent - delays : extent - delays + rows_mix].astype(F32)
        if delays > 0:
            lagged = jnp.where((offset >= delays)[:, None], lagged, 0.0)
        filtered = filtered + conv_taps[extent - delays] * lagged
    mixed = (out_gate.astype(F32) * filtered).astype(BF16)
    pieces = []
    for k in range(tp):
        there = mixed
        if k:
            there = lax.ppermute(mixed, "tp", [(i, (i + k) % tp) for i in range(tp)])
        product = jnp.dot(there, out_weight, preferred_element_type=F32).astype(BF16)
        if k:
            product = lax.ppermute(product, "tp", [((i + k) % tp, i) for i in range(tp)])
        pieces.append(product)
    me = lax.axis_index("tp")
    columns = out_weight.shape[1]
    result = jnp.zeros((rows_mix, tp * columns), BF16)
    for k, piece in enumerate(pieces):
        result = lax.dynamic_update_slice(result, piece, (0, (me + k) % tp * columns))
    return result


def local(
    out_gate,
    in_gate,
    values,
    conv_taps,
    out_weight,
    expert_input,
    norm_gain,
    expert_ids,
    route_logits,
    group_share,
    gate_weight,
    up_weight,
    down_weight,
):
    ep, tp = lax.axis_size("ep"), lax.axis_size("tp")
    planes, across = plane_shape(ep)
    me_ep, me_tp = lax.axis_index("ep"), lax.axis_index("tp")
    z, x = me_ep // across, me_ep % across
    units = gate_weight.shape[2]
    width = expert_input.shape[1]

    def along(value, pairs):
        whole = [(a * across + c, b * across + c) for a, b in pairs for c in range(across)]
        return lax.ppermute(value, "ep", whole)

    margin = route_logits[:, 0] - route_logits[:, 1]
    meta = jnp.stack(
        [
            expert_ids[:, 0].astype(F32),
            expert_ids[:, 1].astype(F32),
            group_share * jax.nn.sigmoid(margin),
            group_share * jax.nn.sigmoid(-margin),
        ]
    )
    meta = lax.all_gather(meta, "ep", axis=0)

    gate, up, down = gate_weight[0], up_weight[0], down_weight[0]
    parts = min(tp, units // LANES)
    others = []
    if across > 1:
        mine = pack_weights(gate, up, down, (me_tp % parts).reshape(1), parts)
        lanes = 2 if parts % 2 == 0 else 1
        for k in range(1, across):
            got = [
                lax.ppermute(
                    piece,
                    "ep",
                    [
                        (a * across + (c + k) % across, a * across + c)
                        for a in range(planes)
                        for c in range(across)
                    ],
                )
                for piece in mine
            ]
            shares = [got]
            for m in range(1, parts // lanes):
                pairs = [
                    (i, i // parts * parts + (i % parts + m * lanes) % parts) for i in range(tp)
                ]
                shares.append([lax.ppermute(piece, "tp", pairs) for piece in got])
            if lanes == 2:
                pairs = [(i, i ^ 1) for i in range(tp)]
                shares += [[lax.ppermute(piece, "tp", pairs) for piece in share] for share in shares]
            others.append(shares)
    experts = jnp.stack([z * across + (x + k) % across for k in range(across)]).astype(jnp.int32)

    gain = norm_gain.reshape(1, width)

    def run(slots):
        scalars = []
        for slot in slots:
            for _, away in slot:
                plane = z + away
                valid = (plane >= 0) & (plane < planes)
                origin = jnp.clip(plane, 0, planes - 1) * across + x
                scalars += [valid.astype(jnp.int32), origin.astype(jnp.int32)]
        return ffn(
            [[array for array, _ in slot] for slot in slots],
            jnp.stack(scalars),
            experts,
            meta,
            gain,
            (gate, up, down),
            others,
        )

    own = expert_input
    low = (planes + 1) // 2
    seen = {}
    for d in range(planes - 1, 2, -1):
        to_low = [(a, a - d) for a in range(d, planes)]
        to_high = [(a, a + d) for a in range(planes - d)]
        if d >= low:
            both = along(own, to_low + to_high)
            seen[d] = (both, both)
        else:
            seen[d] = (along(own, to_low), along(own, to_high))
    if planes > 1:
        seen[1] = (
            along(own, [(a, a - 1) for a in range(1, planes)]),
            along(own, [(a, a + 1) for a in range(planes - 1)]),
        )
    if planes > 2:
        seen[2] = (
            along(seen[1][0], [(a, a - 1) for a in range(1, planes - 1)]),
            along(seen[1][1], [(a, a + 1) for a in range(1, planes - 1)]),
        )

    partial = {}
    for d in range(planes - 1, 2, -1):
        if d >= low:
            partial[d] = run([[(seen[d][0], d), (seen[d][1], -d)]]) * 2
        else:
            partial[d] = run([[(seen[d][0], d)], [(seen[d][1], -d)]])
    near = [[(own, 0)]]
    if planes > 1:
        near += [[(seen[1][0], 1)], [(seen[1][1], -1)]]
    near = run(near)
    if planes > 1:
        partial[1] = near[1:]
    if planes > 2:
        if 2 >= low:
            partial[2] = run([[(seen[2][0], 2), (seen[2][1], -2)]]) * 2
        else:
            partial[2] = run([[(seen[2][0], 2)], [(seen[2][1], -2)]])

    def plus(a, b):
        return (a.astype(F32) + b.astype(F32)).astype(BF16)

    came = None
    for d in range(planes - 1, 0, -1):
        up_pairs = [(a, a + 1) for a in range(planes - d)]
        down_pairs = [(a, a - 1) for a in range(d, planes)]
        if d >= low:
            send = partial[d][0]
            if came is not None:
                send = plus(send, came[0])
            if {b for _, b in up_pairs} & {b for _, b in down_pairs}:
                came = (along(send, up_pairs), along(send, down_pairs))
            else:
                came = (along(send, up_pairs + down_pairs),) * 2
        else:
            send = partial[d]
            if came is not None:
                send = [plus(send[0], came[0]), plus(send[1], came[1])]
            came = (along(send[0], up_pairs), along(send[1], down_pairs))
    total = near[0].astype(F32)
    if came is not None:
        total = total + came[0].astype(F32) + came[1].astype(F32)
    expert_mix = total.astype(BF16)

    mixer_out = mixer(out_gate, in_gate, values, conv_taps, out_weight)
    return (mixer_out, expert_mix)


def solution(mesh):
    return jax.shard_map(
        local,
        mesh=mesh,
        in_specs=(
            P(("ep", "tp"), None),
            P(("ep", "tp"), None),
            P(("ep", "tp"), None),
            P(),
            P(None, "tp"),
            P(("ep", "tp"), None),
            P(),
            P(("ep", "tp"), None),
            P(("ep", "tp"), None),
            P(("ep", "tp")),
            P("ep", None, None),
            P("ep", None, None),
            P("ep", None, None),
        ),
        out_specs=(P(("ep", "tp"), None), P(("ep", "tp"), None)),
        check_vma=False,
    )
```
